32 devices in a mesh: fs: 8 (over z, y), tp: 4 (over x, core).
Axes of the slice: x: 2, y: 2, z: 4, core: 2. Of those that a mesh axis runs over, the one named last changes fastest.
Arguments:
- inputs: bfloat16 [4608, 2048], P('fs'), may hold values from -6 to 6
- query_cotangent: bfloat16 [4608, 1024], P('fs', 'tp'), may hold values from -0.017944336 to 0.017944336
- value_cotangent: bfloat16 [4608, 1024], P('fs', 'tp'), may hold values from -0.017944336 to 0.017944336
- weights_query: float32 [2048, 1024], P('fs', 'tp'), may hold values from -6 to 6
- weights_value: float32 [2048, 1024], P('fs', 'tp'), may hold values from -6 to 6
- basis_query: bfloat16 [1024, 32], P('tp'), may hold values from -0.75 to 0.75
- basis_value: bfloat16 [1024, 32], P('tp'), may hold values from -0.75 to 0.75
- first_query: float32 [2048, 512], P('fs', 'tp'), may hold values from -5.4 to 5.4, as said below
- second_query: float32 [2048, 512], P('fs', 'tp'), may hold values from 0.05 to 1
- first_value: float32 [2048, 512], P('fs', 'tp'), may hold values from -5.4 to 5.4, as said below
- second_value: float32 [2048, 512], P('fs', 'tp'), may hold values from 0.05 to 1
Outputs:
- step_query: float32 [2048, 1024], P('fs', 'tp')
- step_value: float32 [2048, 1024], P('fs', 'tp')
- new_query: float32 [2048, 1024], P('fs', 'tp')
- new_value: float32 [2048, 1024], P('fs', 'tp')
- copy_query: bfloat16 [2048, 1024], P(None, 'tp')
- copy_value: bfloat16 [2048, 1024], P(None, 'tp')
- moment_query: float32 [2048, 512], P('fs', 'tp')
- square_query: float32 [2048, 512], P('fs', 'tp')
- moment_value: float32 [2048, 512], P('fs', 'tp')
- square_value: float32 [2048, 512], P('fs', 'tp')
The draws below stay inside these ranges and needn't reach their ends.
Inputs may be any that keep to these rules, and one draw needn't show every extreme that they name: `first_query`: first moments, with a spread of scale from row to row. `first_value`: first moments, with a spread of scale from row to row.
All inputs are finite; a program needn't handle non-finite values.
Results may differ from the reference program's by a relative error of at most 0.003.
Values may be sent and summed in bfloat16 or wider, within the bound.
No kernel may reach another device: no remote copies, remote signals or barrier semaphores. Data moves between devices by JAX's collectives and lax.ppermute only.
A program may use at most 64 MiB of HBM per device.

```python
import math
import jax
import jax.numpy as jnp
from jax import lax

D = 2048
HEADS = 16
HEAD = 64
RK = 32
FW = 1024
TOKENS = 4608


def moment_draw(key):
    base = 0.3 * jnp.clip(jax.random.normal(jax.random.fold_in(key, 11), (D, HEADS * RK), jnp.float32), -4.0, 4.0)
    factor = jnp.exp(jax.random.uniform(jax.random.fold_in(key, 12), (D, 1), jnp.float32, -1.5, 1.5))
    return base * factor


def draw_first_query(key, part):
    return moment_draw(jax.random.fold_in(key, 1))


def draw_first_value(key, part):
    return moment_draw(jax.random.fold_in(key, 2))


def raised(drawn, own_key, source, target, parts, factor):
    owner, partner = [(jnp.arange(drawn.shape[position]) // (drawn.shape[position] // parts)).reshape([-1 if axis == position else 1 for axis in range(drawn.ndim)]) for position in (source, target)]
    chosen = jax.random.permutation(own_key, parts)[partner]
    strong = (owner == chosen) | (owner == (partner + parts // 2) % parts)
    return jnp.where(strong, factor * drawn, drawn)


def block_levels(rng, shape, cuts, smallest, high):
    level, own = 1.0, jax.random.fold_in(rng, 6)
    for axis_at, shards_of in cuts:
        heights = jnp.exp(jax.random.uniform(jax.random.fold_in(own, axis_at), (shards_of,), jnp.float32, smallest / len(cuts), high / len(cuts)))
        level = level * jnp.repeat(heights, shape[axis_at] // shards_of).reshape([-1 if axis == axis_at else 1 for axis in range(len(shape))])
    return level


def bell_draw(rng, dims, width, bound, cuts=(), held_as=jnp.bfloat16):
    entries = jax.random.normal(rng, dims, jnp.float32) * width
    if len(cuts) > 0:
        entries = block_levels(rng, dims, cuts, -0.22, 0.18) * entries
    return jnp.clip(entries, min=-bound, max=bound).astype(held_as)


def bell_draw_with(rng, extent, width, most, cuts, heavy, dtype=jnp.bfloat16):
    drawn = width * jax.random.normal(rng, extent, jnp.float32)
    if cuts:
        drawn = drawn * block_levels(rng, extent, cuts, -0.22, 0.18)
    return jnp.clip(raised(drawn, jax.random.fold_in(rng, 3), *heavy), -most, most).astype(dtype)


def setup_inputs(seed: int = 0) -> dict:
    key_list = jax.random.split(jax.random.key(seed), 12)
    inputs = bell_draw_with(key_list[0], (TOKENS, D), 1.0, 6.0, ((0, 8),), (0, 1, 8, 2.0))
    query_cotangent = bell_draw(key_list[1], (TOKENS, FW), 0.003, 0.017944336, ((0, 8), (1, 4)))
    value_cotangent = bell_draw(key_list[2], (TOKENS, FW), 0.003, 0.017944336, ((0, 8), (1, 4)))
    weights_query = bell_draw(key_list[3], (D, FW), 1.0, 6.0, ((0, 8), (1, 4)), jnp.float32)
    weights_value = bell_draw(key_list[4], (D, FW), 1.0, 6.0, ((0, 8), (1, 4)), jnp.float32)
    basis_query = bell_draw(key_list[5], (FW, RK), HEAD ** -0.5, 0.75, ((0, 4),))
    basis_value = bell_draw(key_list[6], (FW, RK), HEAD ** -0.5, 0.75, ((0, 4),))
    first_query = draw_first_query(jax.random.fold_in(key_list[11], 71), 0)
    second_query = jnp.clip(jnp.exp(math.log(1.0) - 2.9957323 * jax.random.uniform(key_list[8], (D, HEADS * RK), jnp.float32) ** block_levels(key_list[8], (D, HEADS * RK), ((0, 8), (1, 4)), -0.2, 0.2)), 0.05, 1.0)
    first_value = draw_first_value(jax.random.fold_in(key_list[11], 71), 0)
    second_value = jnp.clip(jnp.exp(math.log(1.0) - 2.9957323 * jax.random.uniform(key_list[10], (D, HEADS * RK), jnp.float32) ** block_levels(key_list[10], (D, HEADS * RK), ((0, 8), (1, 4)), -0.2, 0.2)), 0.05, 1.0)
    return {"inputs": inputs, "query_cotangent": query_cotangent, "value_cotangent": value_cotangent, "weights_query": weights_query, "weights_value": weights_value, "basis_query": basis_query, "basis_value": basis_value, "first_query": first_query, "second_query": second_query, "first_value": first_value, "second_value": second_value}


def apply_basis(gradient, basis):
    split = gradient.reshape(D, HEADS, HEAD)
    factor = basis.reshape(HEADS, HEAD, RK).astype(jnp.float32)
    out = jnp.einsum('nhd,hdr->nhr', split, factor, precision=lax.Precision.HIGHEST)
    return out.reshape(D, HEADS * RK)

def expand(direction, basis):
    split = direction.reshape(D, HEADS, RK)
    factor = basis.reshape(HEADS, HEAD, RK).astype(jnp.float32)
    out = jnp.einsum('nhr,hdr->nhd', split, factor, precision=lax.Precision.HIGHEST)
    return out.reshape(D, HEADS * HEAD)

def update(inputs, cotangent, weights, basis, first, second):
    gradient = jnp.dot(inputs.T, cotangent, preferred_element_type=jnp.float32)
    reduced = apply_basis(gradient, basis)
    moment = 0.9 * first + 0.1 * reduced
    square = 0.95 * second + 0.05 * reduced * reduced
    direction = moment / (jnp.sqrt(square) + 1e-08)
    scale = 1.0 / jnp.sqrt(jnp.mean(direction * direction) + 0.25)
    step = scale * expand(direction, basis)
    fresh = weights - 0.1 * step
    return (step, fresh, fresh.astype(jnp.bfloat16), moment, square)

def reference(inputs, query_cotangent, value_cotangent, weights_query, weights_value, basis_query, basis_value, first_query, second_query, first_value, second_value):
    step_q, new_q, copy_q, moment_q, square_q = update(inputs, query_cotangent, weights_query, basis_query, first_query, second_query)
    step_v, new_v, copy_v, moment_v, square_v = update(inputs, value_cotangent, weights_value, basis_value, first_value, second_value)
    return (step_q, step_v, new_q, new_v, copy_q, copy_v, moment_q, square_q, moment_v, square_v)
```

```python
import functools

import jax
import jax.numpy as jnp
from jax import lax
from jax.experimental import pallas as pl
from jax.experimental.pallas import tpu as pltpu
from jax.sharding import PartitionSpec as P

VMEM = pl.BlockSpec(memory_space=pltpu.VMEM)
ANY = pl.BlockSpec(memory_space=pl.ANY)
TREE_MOST = 8


def code_of(place):
    high = place >> 1
    return ((high ^ (high >> 1)) << 1) | (place & 1)


def place_of(code, bits):
    high = code >> 1
    total = high
    for shift in range(1, bits):
        total = total ^ (high >> shift)
    return (total << 1) | (code & 1)


def link_of(rel, bits):
    for e in range(bits):
        if rel >> e & 1 and (rel >> ((e - 1) % bits) & 1):
            return 1 << e
    return rel & -rel


def by_depth(count):
    return sorted(range(1, count), key=lambda r: -bin(r).count("1"))


def flip(value, bit, count, bits):
    pairs = [(i, place_of(code_of(i) ^ bit, bits)) for i in range(count)]
    return lax.ppermute(value, "fs", pairs)


def spread(bt_ref, head, rank):
    heads = bt_ref.shape[1] // head
    stacked = jnp.concatenate([bt_ref[...]] * heads, axis=0)
    row = lax.broadcasted_iota(jnp.int32, stacked.shape, 0) // rank
    col = lax.broadcasted_iota(jnp.int32, stacked.shape, 1) // head
    return jnp.where(row == col, stacked, jnp.zeros_like(stacked))


def block_of(x_ref, rel, bits, rows):
    place = place_of(code_of(lax.axis_index("fs")) ^ rel, bits)
    return x_ref[:, pl.ds(pl.multiple_of(place * rows, rows), rows)]


def products(hi, lo, block):
    high = jnp.dot(hi, block, preferred_element_type=jnp.float32)
    return high + jnp.dot(lo, block, preferred_element_type=jnp.float32)


def first_kernel(rels, bits, rows, head, rank, x_ref, cq_ref, cv_ref, bq_ref, bv_ref, hi_ref, lo_ref, *outs):
    last = (((1,), (1,)), ((), ()))
    space = bq_ref.shape[1] // head * rank
    for k, (c_ref, b_ref) in enumerate(((cq_ref, bq_ref), (cv_ref, bv_ref))):
        small = lax.dot_general(spread(b_ref, head, rank), c_ref[...], last, preferred_element_type=jnp.float32)
        high = small.astype(jnp.bfloat16)
        hi_ref[k * space : (k + 1) * space, :] = high
        lo_ref[k * space : (k + 1) * space, :] = (small - high.astype(jnp.float32)).astype(jnp.bfloat16)
    for rel, out in zip(rels, outs):
        out[...] = products(hi_ref[...], lo_ref[...], block_of(x_ref, rel, bits, rows)).astype(out.dtype)


def second_kernel(rels, bits, rows, x_ref, hi_ref, lo_ref, *outs):
    for rel, out in zip(rels, outs):
        out[...] = products(hi_ref[...], lo_ref[...], block_of(x_ref, rel, bits, rows)).astype(out.dtype)


def moment_kernel(parts, *refs):
    sums, (fq, sq, fv, sv) = refs[:parts], refs[parts : parts + 4]
    mq, nq, mv, nv, dq, dv, part = refs[parts + 4 :]
    total = sums[0][...]
    for s in sums[1:]:
        total = total + s[...].astype(jnp.float32)
    total = total.T
    space = fq.shape[1]
    for k, (f, s, m, n, d) in enumerate(((fq, sq, mq, nq, dq), (fv, sv, mv, nv, dv))):
        reduced = total[:, k * space : (k + 1) * space]
        moment = 0.9 * f[...] + 0.1 * reduced
        square = 0.95 * s[...] + 0.05 * reduced * reduced
        direction = moment / (jnp.sqrt(square) + 1e-08)
        m[...] = moment
        n[...] = square
        d[...] = direction
        squares = direction * direction
        part[8 * k : 8 * k + 8, :] = jnp.sum(squares.reshape(-1, 8, space), axis=0)


def expand_kernel(head, rank, dq, dv, bq, bv, uq, uv):
    for d, b, u in ((dq, bq, uq), (dv, bv, uv)):
        factor = spread(b, head, rank)
        value = d[...]
        high = value.astype(jnp.bfloat16)
        low = (value - high.astype(jnp.float32)).astype(jnp.bfloat16)
        u[...] = jnp.dot(high, factor, preferred_element_type=jnp.float32) + jnp.dot(
            low, factor, preferred_element_type=jnp.float32
        )


def step_kernel(entries, total, uq, uv, wq, wv, step_q, step_v, new_q, new_v, copy):
    cols = wq.shape[1]
    for k, (u, w, step_ref, new_ref) in enumerate(((uq, wq, step_q, new_q), (uv, wv, step_v, new_v))):
        mean = jnp.sum(total[8 * k : 8 * k + 8, :], keepdims=True) / entries
        step = (1.0 / jnp.sqrt(mean + 0.25)) * u[...]
        fresh = w[...] - 0.1 * step
        step_ref[...] = step
        new_ref[...] = fresh
        copy[:, k * cols : (k + 1) * cols] = fresh.astype(jnp.bfloat16)


def place_kernel(bits, *refs):
    count = 1 << bits
    blocks, (out_q, out_v), sem = refs[:count], refs[count : count + 2], refs[count + 2]
    rows, cols = blocks[0].shape[0], out_q.shape[1]
    mine = code_of(lax.axis_index("fs"))
    copies = []
    for rel in range(count):
        start = pl.multiple_of(place_of(mine ^ rel, bits) * rows, rows)
        for k, out in enumerate((out_q, out_v)):
            copy = pltpu.make_async_copy(
                blocks[rel].at[:, k * cols : (k + 1) * cols], out.at[pl.ds(start, rows), :], sem.at[rel, k]
            )
            copy.start()
            copies.append(copy)
    for copy in copies:
        copy.wait()


def call(kernel, shapes, specs_in, specs_out, flops=0, scratch=()):
    return pl.pallas_call(
        kernel,
        out_shape=shapes,
        in_specs=specs_in,
        out_specs=specs_out,
        scratch_shapes=scratch,
        cost_estimate=pl.CostEstimate(flops=flops, bytes_accessed=0, transcendentals=0) if flops else None,
    )


def across(value, axis, count):
    if count & (count - 1):
        return lax.psum(value, axis)
    bit = 1
    while bit < count:
        value = value + lax.ppermute(value, axis, [(i, i ^ bit) for i in range(count)])
        bit *= 2
    return value


def tree(
    fs_count, tp_count, inputs, query_cotangent, value_cotangent, weights_query, weights_value, basis_query,
    basis_value, first_query, second_query, first_value, second_value,
):
    bits = fs_count.bit_length() - 1
    f32, bf16 = jnp.float32, jnp.bfloat16
    rows, cols = weights_query.shape
    space, rank = first_query.shape[1], basis_query.shape[1]
    head = cols // (space // rank)
    tokens = inputs.shape[0]
    bq, bv = basis_query.T, basis_value.T
    like = jax.ShapeDtypeStruct
    order = by_depth(fs_count)
    fed = {r ^ link_of(r, bits) for r in order}
    leaves = [r for r in order if r not in fed]
    rest = [r for r in order if r in fed] + [0]
    flops = 4 * tokens * 2 * space * rows
    hi, lo, *sent = call(
        functools.partial(first_kernel, leaves, bits, rows, head, rank),
        [like((2 * space, tokens), bf16)] * 2 + [like((2 * space, rows), bf16)] * len(leaves),
        [VMEM] * 5,
        [VMEM] * (2 + len(leaves)),
        flops * len(leaves),
    )(inputs, query_cotangent, value_cotangent, bq, bv)
    kept = call(
        functools.partial(second_kernel, rest, bits, rows),
        [like((2 * space, rows), f32)] * len(rest),
        [VMEM] * 3,
        [VMEM] * len(rest),
        flops * len(rest),
    )(inputs, hi, lo)
    part = dict(zip(rest, kept))
    ready = dict(zip(leaves, sent))
    arrived = {r: [] for r in range(fs_count)}
    for r in order:
        if r not in ready:
            total = part[r]
            for a in arrived[r]:
                total = total + a.astype(f32)
            ready[r] = total.astype(bf16)
        e = link_of(r, bits)
        arrived[r ^ e].append(flip(ready[r], e, fs_count, bits))
    sums = [part[0], *arrived[0]]
    moment_q, square_q, moment_v, square_v, dir_q, dir_v, partial = call(
        functools.partial(moment_kernel, len(sums)),
        [like((rows, space), f32)] * 6 + [like((16, space), f32)],
        [VMEM] * (len(sums) + 4),
        [VMEM] * 7,
    )(*sums, first_query, second_query, first_value, second_value)
    total = across(partial, "tp", tp_count)
    for b in range(bits):
        total = total + flip(total, 1 << b, fs_count, bits)
    u_q, u_v = call(
        functools.partial(expand_kernel, head, rank),
        [like((rows, cols), f32)] * 2,
        [VMEM] * 4,
        [VMEM] * 2,
        8 * rows * space * cols,
    )(dir_q, dir_v, bq, bv)
    entries = fs_count * tp_count * rows * space
    step_q, step_v, new_q, new_v, own = call(
        functools.partial(step_kernel, entries),
        [like((rows, cols), f32)] * 4 + [like((rows, 2 * cols), bf16)],
        [VMEM] * 5,
        [VMEM] * 5,
    )(total, u_q, u_v, weights_query, weights_value)
    blocks = {0: own}
    for r in reversed(order):
        e = link_of(r, bits)
        blocks[r] = flip(blocks[r ^ e], e, fs_count, bits)
    copy_q, copy_v = call(
        functools.partial(place_kernel, bits),
        [like((fs_count * rows, cols), bf16)] * 2,
        [VMEM] * fs_count,
        [ANY] * 2,
        0,
        [pltpu.SemaphoreType.DMA((fs_count, 2))],
    )(*[blocks[r] for r in range(fs_count)])
    return (step_q, step_v, new_q, new_v, copy_q, copy_v, moment_q, square_q, moment_v, square_v)


def plain(
    fs_count, tp_count, inputs, query_cotangent, value_cotangent, weights_query, weights_value, basis_query,
    basis_value, first_query, second_query, first_value, second_value,
):
    rows, cols = weights_query.shape
    space, rank = first_query.shape[1], basis_query.shape[1]
    heads = space // rank
    head = cols // heads
    tokens = inputs.shape[0]
    f32, bf16 = jnp.float32, jnp.bfloat16
    contract = (((0,), (0,)), ((), ()))
    small = jnp.concatenate(
        [
            jnp.einsum(
                "thd,hdr->thr",
                c.reshape(tokens, heads, head),
                b.reshape(heads, head, rank),
                preferred_element_type=f32,
            ).reshape(tokens, space)
            for c, b in ((query_cotangent, basis_query), (value_cotangent, basis_value))
        ],
        axis=1,
    )
    upper = small.astype(bf16)
    lower = (small - upper.astype(f32)).astype(bf16)
    partial = lax.dot_general(inputs, upper, contract, preferred_element_type=f32) + lax.dot_general(
        inputs, lower, contract, preferred_element_type=f32
    )
    reduced = lax.psum_scatter(partial, "fs", scatter_dimension=0, tiled=True)
    results, squares = [], []
    for k, (first, second) in enumerate(((first_query, second_query), (first_value, second_value))):
        own = reduced[:, k * space : (k + 1) * space]
        moment = 0.9 * first + 0.1 * own
        square = 0.95 * second + 0.05 * own * own
        direction = moment / (jnp.sqrt(square) + 1e-08)
        results.append((moment, square, direction))
        squares.append(jnp.sum(direction * direction))
    totals = lax.psum(tuple(squares), ("fs", "tp"))
    entries = fs_count * tp_count * rows * space
    steps, news, copies = [], [], []
    for (_, _, direction), total, basis, weights in zip(
        results, totals, (basis_query, basis_value), (weights_query, weights_value)
    ):
        scale = 1.0 / jnp.sqrt(total / entries + 0.25)
        out = jnp.einsum(
            "nhr,hdr->nhd",
            direction.reshape(rows, heads, rank),
            basis.reshape(heads, head, rank).astype(f32),
            precision=lax.Precision.HIGHEST,
        )
        step = scale * out.reshape(rows, cols)
        fresh = weights - 0.1 * step
        steps.append(step)
        news.append(fresh)
        copies.append(lax.all_gather(fresh.astype(bf16), "fs", axis=0, tiled=True))
    return (*steps, *news, *copies, results[0][0], results[0][1], results[1][0], results[1][1])


def solution(mesh):
    fs_count, tp_count = mesh.shape["fs"], mesh.shape["tp"]
    power = fs_count > 1 and fs_count & (fs_count - 1) == 0
    body = tree if power and fs_count <= TREE_MOST else plain
    both, own = P("fs", "tp"), P("tp", None)
    return jax.shard_map(
        functools.partial(body, fs_count, tp_count),
        mesh=mesh,
        in_specs=(P("fs", None),) + (both,) * 4 + (own,) * 2 + (both,) * 4,
        out_specs=(both,) * 4 + (P(None, "tp"),) * 2 + (both,) * 4,
        check_vma=False,
    )
```

```python
import functools

import jax
import jax.numpy as jnp
from jax import lax
from jax.experimental import pallas as pl
from jax.experimental.pallas import tpu as pltpu
from jax.sharding import PartitionSpec as P

VMEM = pl.BlockSpec(memory_space=pltpu.VMEM)
ANY = pl.BlockSpec(memory_space=pltpu.HBM)
TREE_MOST = 8
KERNEL_BYTES = 16 << 20


def link_of(rel, bits, turn=0):
    top = 1 << (bits - 1)
    if rel == top or rel & (rel - 1) == 0:
        return rel
    if rel & top:
        return rel & -rel
    return rel & -rel if turn else 1 << (rel.bit_length() - 1)


def by_depth(count):
    return sorted(range(1, count), key=lambda r: -bin(r).count("1"))


def flip(value, bit, count):
    pairs = [(i, i ^ bit) for i in range(count)]
    return lax.ppermute(value, "fs", pairs)


def spread(bt_ref, head, rank):
    heads = bt_ref.shape[1] // head
    stacked = jnp.concatenate([bt_ref[...]] * heads, axis=0)
    row = lax.broadcasted_iota(jnp.int32, stacked.shape, 0) // rank
    col = lax.broadcasted_iota(jnp.int32, stacked.shape, 1) // head
    return jnp.where(row == col, stacked, jnp.zeros_like(stacked))


def span_of(rel, rows):
    return pl.ds(pl.multiple_of((lax.axis_index("fs") ^ rel) * rows, rows), rows)


def products(hi, lo, block):
    high = jnp.dot(hi, block, preferred_element_type=jnp.float32)
    return high + jnp.dot(lo, block, preferred_element_type=jnp.float32)


def first_kernel(
    rels, count, rows, head, rank, x_all, cq_all, cv_all, bq_all, bv_all, x_ref, bq_ref, bv_ref, hi_ref, lo_ref, *refs
):
    outs, (cq_ref, cv_ref, small_sem, x_sem) = refs[: len(rels)], refs[len(rels) :]
    small = [
        pltpu.make_async_copy(src, dst, small_sem.at[i])
        for i, (src, dst) in enumerate(
            ((bq_all, bq_ref), (cq_all, cq_ref), (bv_all, bv_ref), (cv_all, cv_ref))
        )
    ]
    for copy in small:
        copy.start()
    order = [*rels, *[r for r in range(count) if r not in rels]]
    blocks = {r: pltpu.make_async_copy(x_all.at[:, span_of(r, rows)], x_ref.at[:, span_of(r, rows)], x_sem.at[r]) for r in order}
    for r in order:
        blocks[r].start()
    last = (((1,), (1,)), ((), ()))
    space = bq_ref.shape[1] // head * rank
    for k, (c_ref, b_ref) in enumerate(((cq_ref, bq_ref), (cv_ref, bv_ref))):
        small[2 * k].wait()
        small[2 * k + 1].wait()
        value = lax.dot_general(spread(b_ref, head, rank), c_ref[...], last, preferred_element_type=jnp.float32)
        high = value.astype(jnp.bfloat16)
        hi_ref[k * space : (k + 1) * space, :] = high
        lo_ref[k * space : (k + 1) * space, :] = (value - high.astype(jnp.float32)).astype(jnp.bfloat16)
    for rel, out in zip(rels, outs):
        blocks[rel].wait()
        out[...] = products(hi_ref[...], lo_ref[...], x_ref[:, span_of(rel, rows)]).astype(out.dtype)
    for r in order[len(rels) :]:
        blocks[r].wait()


def second_kernel(rels, rows, x_ref, hi_ref, lo_ref, *outs):
    for rel, out in zip(rels, outs):
        out[...] = products(hi_ref[...], lo_ref[...], x_ref[:, span_of(rel, rows)]).astype(out.dtype)


def moment_kernel(parts, *refs):
    sums, (fq, sq, fv, sv) = refs[:parts], refs[parts : parts + 4]
    mq, nq, mv, nv, dq, dv, part = refs[parts + 4 :]
    total = sums[0][...]
    for s in sums[1:]:
        total = total + s[...].astype(jnp.float32)
    total = total.T
    space = fq.shape[1]
    for k, (f, s, m, n, d) in enumerate(((fq, sq, mq, nq, dq), (fv, sv, mv, nv, dv))):
        reduced = total[:, k * space : (k + 1) * space]
        moment = 0.9 * f[...] + 0.1 * reduced
        square = 0.95 * s[...] + 0.05 * reduced * reduced
        direction = moment / (jnp.sqrt(square) + 1e-08)
        m[...] = moment
        n[...] = square
        d[...] = direction
        squares = direction * direction
        part[8 * k : 8 * k + 8, :] = jnp.sum(squares.reshape(-1, 8, space), axis=0)


def step_kernel(entries, head, rank, sum_a, sum_b, dq, dv, bq, bv, wq, wv, step_q, step_v, new_q, new_v, copy_q, copy_v):
    total = sum_a[...] + sum_b[...]
    for k, (d, b, w, step_ref, new_ref, copy) in enumerate(
        ((dq, bq, wq, step_q, new_q, copy_q), (dv, bv, wv, step_v, new_v, copy_v))
    ):
        factor = spread(b, head, rank)
        value = d[...]
        high = value.astype(jnp.bfloat16)
        low = (value - high.astype(jnp.float32)).astype(jnp.bfloat16)
        out = jnp.dot(high, factor, preferred_element_type=jnp.float32) + jnp.dot(
            low, factor, preferred_element_type=jnp.float32
        )
        mean = jnp.sum(total[8 * k : 8 * k + 8, :], keepdims=True) / entries
        step = (1.0 / jnp.sqrt(mean + 0.25)) * out
        fresh = w[...] - 0.1 * step
        step_ref[...] = step
        new_ref[...] = fresh
        copy[...] = fresh.astype(jnp.bfloat16)


def place_kernel(rels, plain, held, *refs):
    blocks, others = refs[: len(rels)], refs[len(rels) : len(rels) + plain]
    outs = refs[len(rels) + plain + (2 if held else 0) : -1]
    sem = refs[-1]
    moves = []
    for i, (which, rel) in enumerate(rels):
        moves.append((blocks[i], outs[which].at[span_of(rel, blocks[i].shape[0]), :]))
    moves += zip(others, outs[2:])
    copies = [pltpu.make_async_copy(src, dst, sem.at[i]) for i, (src, dst) in enumerate(moves)]
    for copy in copies:
        copy.start()
    for copy in copies:
        copy.wait()


def call(kernel, shapes, specs_in, specs_out, flops=0, scratch=(), aliases=None):
    return pl.pallas_call(
        kernel,
        out_shape=shapes,
        in_specs=specs_in,
        out_specs=specs_out,
        scratch_shapes=scratch,
        input_output_aliases=aliases or {},
        compiler_params=pltpu.CompilerParams(vmem_limit_bytes=KERNEL_BYTES),
        cost_estimate=pl.CostEstimate(flops=flops, bytes_accessed=0, transcendentals=0) if flops else None,
    )


def near(value):
    return pltpu.with_memory_space_constraint(value, pltpu.VMEM)


def far(value):
    return pltpu.with_memory_space_constraint(value, pltpu.HBM)


def across(value, axis, count):
    if count & (count - 1):
        return lax.psum(value, axis)
    bit = 1
    while bit < count:
        value = value + lax.ppermute(value, axis, [(i, i ^ bit) for i in range(count)])
        bit *= 2
    return value


def tree(
    fs_count, tp_count, inputs, query_cotangent, value_cotangent, weights_query, weights_value, basis_query,
    basis_value, first_query, second_query, first_value, second_value,
):
    bits = fs_count.bit_length() - 1
    f32, bf16 = jnp.float32, jnp.bfloat16
    rows, cols = weights_query.shape
    space, rank = first_query.shape[1], basis_query.shape[1]
    head = cols // (space // rank)
    tokens = inputs.shape[0]
    bq, bv = basis_query.T, basis_value.T
    like = jax.ShapeDtypeStruct
    order = by_depth(fs_count)
    fed = {r ^ link_of(r, bits) for r in order}
    first, rest = order[:1], [*order[1:], 0]
    flops = 4 * tokens * 2 * space * rows
    wide, narrow = pltpu.VMEM((2 * space, tokens), bf16), pltpu.VMEM(bq.shape, bf16)
    x, bq, bv, hi, lo, *sent = call(
        functools.partial(first_kernel, first, fs_count, rows, head, rank),
        [pltpu.VMEM(inputs.shape, bf16), narrow, narrow, wide, wide]
        + [pltpu.VMEM((2 * space, rows), bf16)] * len(first),
        [ANY] * 5,
        [VMEM] * (5 + len(first)),
        flops * len(first),
        [pltpu.VMEM((tokens, cols), bf16)] * 2
        + [pltpu.SemaphoreType.DMA((4,)), pltpu.SemaphoreType.DMA((fs_count,))],
    )(*[far(v) for v in (inputs, query_cotangent, value_cotangent, bq, bv)])
    others = call(
        functools.partial(second_kernel, rest, rows),
        [pltpu.VMEM((2 * space, rows), f32 if r in fed else bf16) for r in rest],
        [VMEM] * 3,
        [VMEM] * len(rest),
        flops * len(rest),
    )(near(x), near(hi), near(lo))
    part = {**dict(zip(first, sent)), **dict(zip(rest, others))}
    arrived = {r: [] for r in range(fs_count)}
    for r in order:
        total = part[r]
        for a in arrived[r]:
            total = total + a.astype(f32)
        e = link_of(r, bits)
        arrived[r ^ e].append(flip(total.astype(bf16), e, fs_count))
    sums = [part[0], *arrived[0]]
    moment_q, square_q, moment_v, square_v, dir_q, dir_v, partial = call(
        functools.partial(moment_kernel, len(sums)),
        [pltpu.VMEM((rows, space), f32)] * 6 + [pltpu.VMEM((16, space), f32)],
        [VMEM] * (len(sums) + 4),
        [VMEM] * 7,
    )(*[near(v) for v in (*sums, first_query, second_query, first_value, second_value)])
    total = across(partial, "tp", tp_count)
    for b in range(bits - 1):
        total = total + flip(total, 1 << b, fs_count)
    other = flip(total, 1 << (bits - 1), fs_count)
    entries = fs_count * tp_count * rows * space
    step_q, step_v, new_q, new_v, *own = call(
        functools.partial(step_kernel, entries, head, rank),
        [pltpu.VMEM((rows, cols), f32)] * 4 + [pltpu.VMEM((rows, cols), bf16)] * 2,
        [VMEM] * 8,
        [VMEM] * 6,
        8 * rows * space * cols,
    )(*[near(v) for v in (total, other, dir_q, dir_v, bq, bv, weights_query, weights_value)])
    blocks = {(k, 0): own[k] for k in range(2)}
    for r in reversed(order):
        for k in range(2):
            e = link_of(r, bits, k)
            blocks[k, r] = flip(blocks[k, r ^ e], e, fs_count)
    early = [key for key in blocks if key[1] != fs_count - 1]
    late = [key for key in blocks if key[1] == fs_count - 1]
    shapes = [like((fs_count * rows, cols), bf16)] * 2
    done = [step_q, step_v, new_q, new_v, moment_q, square_q, moment_v, square_v]
    copy_q, copy_v, *done = call(
        functools.partial(place_kernel, early, len(done), False),
        shapes + [like(v.shape, v.dtype) for v in done],
        [VMEM] * (len(early) + len(done)),
        [ANY] * (2 + len(done)),
        2 * cols * rows * fs_count,
        [pltpu.SemaphoreType.DMA((len(early) + len(done),))],
    )(*[near(blocks[key]) for key in early], *[near(v) for v in done])
    copy_q, copy_v = call(
        functools.partial(place_kernel, late, 0, True),
        shapes,
        [VMEM] * len(late) + [ANY] * 2,
        [ANY] * 2,
        0,
        [pltpu.SemaphoreType.DMA((len(late),))],
        {len(late): 0, len(late) + 1: 1},
    )(*[near(blocks[key]) for key in late], copy_q, copy_v)
    return (*done[:4], copy_q, copy_v, *done[4:])


def plain(
    fs_count, tp_count, inputs, query_cotangent, value_cotangent, weights_query, weights_value, basis_query,
    basis_value, first_query, second_query, first_value, second_value,
):
    rows, cols = weights_query.shape
    space, rank = first_query.shape[1], basis_query.shape[1]
    heads = space // rank
    head = cols // heads
    tokens = inputs.shape[0]
    f32, bf16 = jnp.float32, jnp.bfloat16
    contract = (((0,), (0,)), ((), ()))
    small = jnp.concatenate(
        [
            jnp.einsum(
                "thd,hdr->thr",
                c.reshape(tokens, heads, head),
                b.reshape(heads, head, rank),
                preferred_element_type=f32,
            ).reshape(tokens, space)
            for c, b in ((query_cotangent, basis_query), (value_cotangent, basis_value))
        ],
        axis=1,
    )
    upper = small.astype(bf16)
    lower = (small - upper.astype(f32)).astype(bf16)
    partial = lax.dot_general(inputs, upper, contract, preferred_element_type=f32) + lax.dot_general(
        inputs, lower, contract, preferred_element_type=f32
    )
    reduced = lax.psum_scatter(partial, "fs", scatter_dimension=0, tiled=True)
    results, squares = [], []
    for k, (first, second) in enumerate(((first_query, second_query), (first_value, second_value))):
        own = reduced[:, k * space : (k + 1) * space]
        moment = 0.9 * first + 0.1 * own
        square = 0.95 * second + 0.05 * own * own
        direction = moment / (jnp.sqrt(square) + 1e-08)
        results.append((moment, square, direction))
        squares.append(jnp.sum(direction * direction))
    totals = lax.psum(tuple(squares), ("fs", "tp"))
    entries = fs_count * tp_count * rows * space
    steps, news, copies = [], [], []
    for (_, _, direction), total, basis, weights in zip(
        results, totals, (basis_query, basis_value), (weights_query, weights_value)
    ):
        scale = 1.0 / jnp.sqrt(total / entries + 0.25)
        out = jnp.einsum(
            "nhr,hdr->nhd",
            direction.reshape(rows, heads, rank),
            basis.reshape(heads, head, rank).astype(f32),
            precision=lax.Precision.HIGHEST,
        )
        step = scale * out.reshape(rows, cols)
        fresh = weights - 0.1 * step
        steps.append(step)
        news.append(fresh)
        copies.append(lax.all_gather(fresh.astype(bf16), "fs", axis=0, tiled=True))
    return (*steps, *news, *copies, results[0][0], results[0][1], results[1][0], results[1][1])


def solution(mesh):
    fs_count, tp_count = mesh.shape["fs"], mesh.shape["tp"]
    power = fs_count > 1 and fs_count & (fs_count - 1) == 0
    body = tree if power and fs_count <= TREE_MOST else plain
    both, own = P("fs", "tp"), P("tp", None)
    return jax.shard_map(
        functools.partial(body, fs_count, tp_count),
        mesh=mesh,
        in_specs=(P("fs", None),) + (both,) * 4 + (own,) * 2 + (both,) * 4,
        out_specs=(both,) * 4 + (P(None, "tp"),) * 2 + (both,) * 4,
        check_vma=False,
    )
```
